32 devices in a mesh: grp: 2 (over y), sp: 4 (over z), tp: 4 (over x, core).
Axes of the slice: x: 2, y: 2, z: 4, core: 2. Of those that a mesh axis runs over, the one named last changes fastest.
Arguments:
- residual: bfloat16 [3072, 2048], P(('grp', 'sp', 'tp')), parts along dimension 0, may hold values from -36 to 36
- query: bfloat16 [3072, 512], P(('grp', 'sp'), 'tp'), parts along dimension 0, may hold values from -6 to 6
- keys: bfloat16 [3072, 512], P(('grp', 'sp'), 'tp'), parts along dimension 0, may hold values from -6 to 6
- values: bfloat16 [3072, 1024], P(('grp', 'sp'), 'tp'), parts along dimension 0, may hold values from -6 to 6
- out_gate: bfloat16 [3072, 1024], P(('grp', 'sp'), 'tp'), parts along dimension 0, may hold values from -6 to 6
- input_gate: float32 [2, 4, 3072], P(None, 'tp', ('grp', 'sp')), parts along dimension 2, may hold values from -5 to 95
- forget_gate: float32 [2, 4, 3072], P(None, 'tp', ('grp', 'sp')), parts along dimension 2, may hold values from -6 to 20
- head_gain: float32 [1024], P('tp'), may hold values from 0.1 to 1.9
- w_out: bfloat16 [1024, 2048], P('tp'), may hold values from -0.1875 to 0.1875
- norm_gain: float32 [2048], replicated, may hold values from 0.1 to 1.9
- w_up_gate: bfloat16 [2048, 5632], P('sp', 'tp'), may hold values from -0.125 to 0.125
- w_up_value: bfloat16 [2048, 5632], P('sp', 'tp'), may hold values from -0.125 to 0.125
- conv_gate: float32 [3, 5632], P(None, 'tp'), may hold values from -3 to 3
- conv_value: float32 [3, 5632], P(None, 'tp'), may hold values from -3 to 3
- w_down: bfloat16 [5632, 2048], P('tp', 'sp'), may hold values from -0.078125 to 0.078125
Outputs:
- layer_out: bfloat16 [3072, 2048], P(('grp', 'sp', 'tp')), parts along dimension 0
The draws below stay inside these ranges and needn't reach their ends.
There are 2 independent parts, one for each index of `grp`. The reference program is written for one: setup_inputs(seed, part) draws one part's arguments, and reference() takes and returns one part's arrays. A program takes and returns all parts, laid end to end along the dimension named above; an argument that names none is the same for every part. Nothing has to cross between parts.
All inputs are finite; a program needn't handle non-finite values.
Results may differ from the reference program's by a relative error of at most 0.011.
Values may be sent and summed in bfloat16 or wider, within the bound.
No kernel may reach another device: no remote copies, remote signals or barrier semaphores. Data moves between devices by JAX's collectives and lax.ppermute only.
A program may use at most 128 MiB of HBM per device.

```python
import math
import jax
import jax.numpy as jnp
from jax import lax

D = 2048
HEADS = 4
QK_DIM = 128
V_DIM = 256
FF = 5632
CONV = 3
TOK_DEV = 384
TOKENS = 1536
QK_WIDTH = 512
V_WIDTH = 1024


def spike_flags(key, item_count):
    spots = jax.random.randint(key, (2, HEADS, item_count), 0, TOKENS)
    places = jnp.arange(TOKENS)
    return jnp.any(places[None, None, :, None] == spots[:, :, None, :], axis=-1)


def draw_input_gate(key, part):
    sequence_lanes = jax.random.split(jax.random.fold_in(key, 11), 1)
    reference_level = jnp.clip(jax.random.normal(sequence_lanes[0], (2, HEADS, TOKENS), jnp.float32), -5.0, 5.0)
    return reference_level


def draw_forget_gate(key, part):
    sequence_lanes = jax.random.split(jax.random.fold_in(key, 23), 6)
    ranking = jnp.stack([jax.random.permutation(sequence_lanes[0], HEADS), jax.random.permutation(sequence_lanes[1], HEADS)])
    quick_heads = ranking < HEADS // 2
    head_rates = jnp.where(quick_heads, 8.0 / TOK_DEV, 0.5 / TOKENS).astype(jnp.float32)
    factor = jnp.exp(jax.random.uniform(sequence_lanes[2], (2, HEADS, TOKENS // TOK_DEV), jnp.float32, -math.log(2.0), math.log(2.0)))
    factor = jnp.repeat(factor, TOK_DEV, axis=2)
    jitter = jnp.clip(jax.random.normal(sequence_lanes[3], (2, HEADS, TOKENS), jnp.float32), -4.0, 4.0)
    stable_value = -jnp.log(head_rates[:, :, None] * factor) - 0.5 + jitter
    retained_state = jax.random.uniform(sequence_lanes[5], (2, HEADS, TOKENS), jnp.float32, 0.5, 0.8)
    return jnp.where(spike_flags(sequence_lanes[4], 3), jnp.log(retained_state / (1.0 - retained_state)), stable_value)


def draw_residual(key, part):
    sequence_lanes = jax.random.split(jax.random.fold_in(key, 37), 3)
    row_scale = jnp.exp(jax.random.uniform(sequence_lanes[0], (TOKENS, 1), jnp.float32, math.log(0.3), math.log(3.0)))
    column_scale = jnp.exp(jax.random.uniform(sequence_lanes[1], (1, D), jnp.float32, math.log(0.3), math.log(3.0)))
    entries = jnp.clip(jax.random.normal(sequence_lanes[2], (TOKENS, D), jnp.float32), -4.0, 4.0)
    return (entries * row_scale * column_scale).astype(jnp.bfloat16)


def levels(key, extent, cuts, low, high):
    level, own = 1.0, jax.random.fold_in(key, 6)
    for position, parts in cuts:
        draws = jnp.exp(jax.random.uniform(jax.random.fold_in(own, position), (parts,), jnp.float32, low / len(cuts), high / len(cuts)))
        level = level * jnp.repeat(draws, extent[position] // parts).reshape([-1 if axis == position else 1 for axis in range(len(extent))])
    return level


def normal_values(stream_key, extent, spread, limit, cuts=(), held_as=jnp.bfloat16):
    level = levels(stream_key, extent, cuts, -0.22, 0.18) if cuts else 1.0
    drawn = jax.random.normal(stream_key, extent, jnp.float32) * spread * level
    return jnp.minimum(jnp.maximum(drawn, -limit), limit).astype(held_as)


def setup_inputs(seed: int = 0, part: int = 0) -> dict:
    key_list = jax.random.split(jax.random.key(seed), 16)
    part_keys = jax.random.split(jax.random.fold_in(key_list[15], part), 16)
    residual = draw_residual(jax.random.fold_in(jax.random.fold_in(key_list[15], part), 71), part)
    query = normal_values(part_keys[1], (TOKENS, QK_WIDTH), 1.0, 6.0, ((0, 4), (1, 4)))
    keys = normal_values(part_keys[2], (TOKENS, QK_WIDTH), 1.0, 6.0, ((0, 4), (1, 4)))
    values = normal_values(part_keys[3], (TOKENS, V_WIDTH), 1.0, 6.0, ((0, 4), (1, 4)))
    out_gate = normal_values(part_keys[4], (TOKENS, V_WIDTH), 1.5, 6.0, ((0, 4), (1, 4)))
    input_gate = draw_input_gate(jax.random.fold_in(jax.random.fold_in(key_list[15], part), 71), part)
    forget_gate = draw_forget_gate(jax.random.fold_in(jax.random.fold_in(key_list[15], part), 71), part)
    head_gain = jnp.clip(1.0 + 0.18 * jax.random.normal(key_list[7], (V_WIDTH,), jnp.float32), 0.1, 1.9)
    w_out = normal_values(key_list[8], (V_WIDTH, D), V_WIDTH ** -0.5, 0.1875, ((0, 4),))
    norm_gain = jnp.clip(1.0 + 0.18 * jax.random.normal(key_list[9], (D,), jnp.float32), 0.1, 1.9)
    w_up_gate = normal_values(key_list[10], (D, FF), D ** -0.5, 0.125, ((0, 4), (1, 4)))
    w_up_value = normal_values(key_list[11], (D, FF), D ** -0.5, 0.125, ((0, 4), (1, 4)))
    conv_gate = normal_values(key_list[12], (CONV, FF), 0.577, 3.0, ((1, 4),), jnp.float32)
    conv_value = normal_values(key_list[13], (CONV, FF), 0.577, 3.0, ((1, 4),), jnp.float32)
    w_down = normal_values(key_list[14], (FF, D), FF ** -0.5, 0.078125, ((0, 4), (1, 4)))
    return {"residual": residual, "query": query, "keys": keys, "values": values, "out_gate": out_gate, "input_gate": input_gate, "forget_gate": forget_gate, "head_gain": head_gain, "w_out": w_out, "norm_gain": norm_gain, "w_up_gate": w_up_gate, "w_up_value": w_up_value, "conv_gate": conv_gate, "conv_value": conv_value, "w_down": w_down}


epsilon = 1e-06
floor_log = -1e+30
highest = lax.Precision.HIGHEST

def summarize(keys_scaled, values_wide, in_gate, log_cum):
    totals = log_cum[:, -1]
    growth = totals[:, None] - log_cum + in_gate
    largest = lax.optimization_barrier(jnp.max(growth, axis=-1))
    weighting = jnp.exp(growth - largest[:, None])
    weighted = keys_scaled * jnp.transpose(weighting)[:, :, None]
    memory = jnp.einsum('shd,she->hde', weighted, values_wide, precision=highest)
    return (totals, memory, lax.optimization_barrier(jnp.sum(weighted, axis=0)), largest)

def combine(early, later):
    early_total, early_memory, early_normalizer, early_top = early
    later_total, later_memory, later_normalizer, later_top = later
    carried = early_top + later_total
    joint_top = jnp.maximum(carried, later_top)
    early_scale = jnp.exp(carried - joint_top)
    later_scale = jnp.exp(later_top - joint_top)
    memory = early_scale[:, None, None] * early_memory + later_scale[:, None, None] * later_memory
    normalizer = early_scale[:, None] * early_normalizer + later_scale[:, None] * later_normalizer
    return (early_total + later_total, memory, normalizer, joint_top)

def read_out(query_wide, keys_wide, values_wide, in_gate, log_cum, state):
    memory, normalizer, top_in = (state[1], state[2], state[3])
    length = query_wide.shape[0]
    lower_tri = jnp.tril(jnp.ones((length, length), dtype=bool))
    exponent = jnp.where(lower_tri[None], log_cum[:, :, None] - log_cum[:, None, :] + in_gate[:, None, :], -jnp.inf)
    before = log_cum + top_in[:, None]
    running = jnp.maximum(before, lax.optimization_barrier(jnp.max(exponent, axis=-1)))
    carry_scale = jnp.exp(before - running)
    scores = jnp.einsum('thd,shd->hts', query_wide, keys_wide, precision=highest) * QK_DIM ** (-0.5)
    weights = jnp.exp(exponent - running[:, :, None]) * scores
    rounded = lax.optimization_barrier(weights.astype(jnp.bfloat16)).astype(jnp.float32)
    numerator = carry_scale[:, :, None] * jnp.einsum('thd,hde->hte', query_wide, memory, precision=highest)
    numerator = numerator + jnp.einsum('hts,she->hte', rounded, values_wide, precision=highest)
    denominator = carry_scale * jnp.einsum('thd,hd->ht', query_wide, normalizer, precision=highest) + lax.optimization_barrier(jnp.sum(weights, axis=-1))
    return numerator / jnp.maximum(jnp.abs(denominator), jnp.exp(-running))[:, :, None]

def one_direction(query_wide, keys_wide, values_wide, in_gate, forget_pre):
    blocks = TOKENS // TOK_DEV
    head_count = in_gate.shape[0]
    log_keep = jax.nn.log_sigmoid(forget_pre)

    def cut_rows(array):
        return array.reshape((blocks, TOK_DEV) + array.shape[1:])

    def cut_gate(array):
        return jnp.moveaxis(array.reshape(head_count, blocks, TOK_DEV), 1, 0)
    initial = (jnp.zeros((head_count,), jnp.float32), jnp.zeros((head_count, QK_DIM, V_DIM), jnp.float32), jnp.zeros((head_count, QK_DIM), jnp.float32), jnp.full((head_count,), floor_log, jnp.float32))

    def advance(state, piece):
        query_block, keys_block, values_block, gate_block, keep_block = piece
        log_cum = jnp.cumsum(keep_block, axis=-1)
        result = read_out(query_block, keys_block, values_block, gate_block, log_cum, state)
        summary = summarize(keys_block * QK_DIM ** (-0.5), values_block, gate_block, log_cum)
        return (combine(state, summary), result)
    _, results = lax.scan(advance, initial, (cut_rows(query_wide), cut_rows(keys_wide), cut_rows(values_wide), cut_gate(in_gate), cut_gate(log_keep)))
    return jnp.moveaxis(results, 0, 1).reshape(head_count, TOKENS, V_DIM)

def smear(upper, taps):
    side = CONV // 2
    padded = jnp.pad(upper.astype(jnp.float32), ((side, CONV - 1 - side), (0, 0)))
    total = padded[0:TOKENS] * taps[0]
    for offset in range(1, CONV):
        total = total + padded[offset:offset + TOKENS] * taps[offset]
    return total

def reference(residual, query, keys, values, out_gate, input_gate, forget_gate, head_gain, w_out, norm_gain, w_up_gate, w_up_value, conv_gate, conv_value, w_down):
    query_wide = query.astype(jnp.float32).reshape(TOKENS, HEADS, QK_DIM)
    keys_wide = keys.astype(jnp.float32).reshape(TOKENS, HEADS, QK_DIM)
    values_wide = values.astype(jnp.float32).reshape(TOKENS, HEADS, V_DIM)
    forward = one_direction(query_wide, keys_wide, values_wide, input_gate[0], forget_gate[0])
    backward = one_direction(jnp.flip(query_wide, axis=0), jnp.flip(keys_wide, axis=0), jnp.flip(values_wide, axis=0), jnp.flip(input_gate[1], axis=-1), jnp.flip(forget_gate[1], axis=-1))
    both = forward + jnp.flip(backward, axis=1)
    scaled = both * lax.rsqrt(lax.optimization_barrier(jnp.mean(both * both, axis=-1, keepdims=True)) + epsilon)
    scaled = scaled * head_gain.reshape(HEADS, V_DIM)[:, None, :]
    side_by_side = jnp.transpose(scaled, (1, 0, 2)).reshape(TOKENS, V_WIDTH)
    gated = (side_by_side * jax.nn.sigmoid(out_gate.astype(jnp.float32))).astype(jnp.bfloat16)
    stream = (residual.astype(jnp.float32) + jnp.dot(gated, w_out, preferred_element_type=jnp.float32)).astype(jnp.bfloat16)
    stream_wide = stream.astype(jnp.float32)
    normed = stream_wide * lax.rsqrt(lax.optimization_barrier(jnp.mean(stream_wide * stream_wide, axis=-1, keepdims=True)) + epsilon)
    normed = (normed * norm_gain).astype(jnp.bfloat16)
    up_gate = jnp.dot(normed, w_up_gate, preferred_element_type=jnp.float32).astype(jnp.bfloat16)
    up_value = jnp.dot(normed, w_up_value, preferred_element_type=jnp.float32).astype(jnp.bfloat16)
    hidden = (jax.nn.silu(smear(up_gate, conv_gate)) * smear(up_value, conv_value)).astype(jnp.bfloat16)
    return (stream_wide + jnp.dot(hidden, w_down, preferred_element_type=jnp.float32)).astype(jnp.bfloat16)
```

```python
import jax
import jax.numpy as jnp
from jax import lax
from jax.sharding import PartitionSpec as P

QK_DIM = 128
V_DIM = 256
CONV = 3


epsilon = 1e-06
floor_log = -1e30
highest = lax.Precision.HIGHEST


def swap(x, axis, distance):
    size = lax.axis_size(axis)
    return lax.ppermute(x, axis, [(i, i ^ distance) for i in range(size)])


def shifted(x, axis, distance):
    size = lax.axis_size(axis)
    pairs = [(i, i + distance) for i in range(size) if 0 <= i + distance < size]
    return lax.ppermute(x, axis, pairs)


def pick(x, index, dim):
    return lax.dynamic_index_in_dim(x, index, axis=dim, keepdims=False)


def in_order(mine, other, bit, dim):
    first = jnp.where(bit == 0, mine, other)
    second = jnp.where(bit == 0, other, mine)
    return jnp.stack([first, second], axis=dim)


def combine(early, later):
    early_total, early_memory, early_normalizer, early_top = early
    later_total, later_memory, later_normalizer, later_top = later
    carried = early_top + later_total
    joint_top = jnp.maximum(carried, later_top)
    early_scale = jnp.exp(carried - joint_top)
    later_scale = jnp.exp(later_top - joint_top)
    memory = early_scale[:, None, None] * early_memory + later_scale[:, None, None] * later_memory
    normalizer = early_scale[:, None] * early_normalizer + later_scale[:, None] * later_normalizer
    return (early_total + later_total, memory, normalizer, joint_top)


def pack(state):
    total, memory, normalizer, top = state
    heads, _, width = memory.shape
    row = jnp.pad(normalizer, ((0, 0), (0, width - normalizer.shape[1])))
    scalars = jnp.pad(jnp.stack([total, top], axis=1), ((0, 0), (0, width - 2)))
    extra = jnp.stack([row, scalars], axis=1)
    return jnp.concatenate([memory, jnp.pad(extra, ((0, 0), (0, 6), (0, 0)))], axis=1)


def unpack(packed, present):
    memory = packed[:, :QK_DIM]
    normalizer = packed[:, QK_DIM, :QK_DIM]
    total = packed[:, QK_DIM + 1, 0]
    top = jnp.where(present, packed[:, QK_DIM + 1, 1], floor_log)
    return (total, memory, normalizer, top)


def entering(state, axis, sign):
    size, mine = lax.axis_size(axis), lax.axis_index(axis)
    place = mine if sign > 0 else size - 1 - mine
    packed = pack(state)
    if size <= 4:
        parts = [unpack(shifted(packed, axis, sign * d), place >= d) for d in range(1, size)]
        result = parts[0]
        for part in parts[1:]:
            result = combine(part, result)
        return result
    result = unpack(shifted(packed, axis, sign), place >= 1)
    reach, step = 1, 1
    while reach < size - 1:
        part = unpack(shifted(pack(result), axis, sign * step), place >= step + 1)
        result = combine(part, result)
        reach += step
        step = reach
    return result


def summarize(keys_scaled, values_wide, in_gate, log_cum, totals):
    growth = totals[:, None] - log_cum + in_gate
    largest = jnp.max(growth, axis=-1)
    weighting = jnp.exp(growth - largest[:, None])
    weighted = keys_scaled * jnp.transpose(weighting)[:, :, None]
    memory = jnp.einsum("shd,she->hde", weighted, values_wide, precision=highest)
    return (totals, memory, jnp.sum(weighted, axis=0), largest)


def own_block(in_gate, log_cum, mask):
    exponent = jnp.where(
        mask[None], log_cum[:, :, None] - log_cum[:, None, :] + in_gate[:, None, :], -jnp.inf
    )
    return exponent, jnp.max(exponent, axis=-1)


def read_out(query_wide, scores, value_heads, exponent, block_top, log_cum, state):
    memory, normalizer, top_in = (state[1], state[2], state[3])
    before = log_cum + top_in[:, None]
    running = jnp.maximum(before, block_top)
    carry_scale = jnp.exp(before - running)
    weights = jnp.exp(exponent - running[:, :, None]) * scores
    numerator = carry_scale[:, :, None] * jnp.einsum(
        "thd,hde->hte", query_wide, memory, precision=highest
    )
    numerator = numerator + jnp.einsum(
        "hts,she->hte",
        weights.astype(jnp.bfloat16),
        value_heads,
        preferred_element_type=jnp.float32,
    )
    denominator = carry_scale * jnp.einsum(
        "thd,hd->ht", query_wide, normalizer, precision=highest
    ) + jnp.sum(weights, axis=-1)
    return numerator / jnp.maximum(jnp.abs(denominator), jnp.exp(-running))[:, :, None]


def heads_part(query, keys, values, out_gate, input_gate, forget_gate, head_gain):
    length = query.shape[0]
    heads_here = input_gate.shape[1]
    query_heads = query.reshape(length, heads_here, QK_DIM)
    keys_heads = keys.reshape(length, heads_here, QK_DIM)
    value_heads = values.reshape(length, heads_here, V_DIM)
    keys_scaled = keys_heads.astype(jnp.float32) * QK_DIM ** (-0.5)
    values_wide = value_heads.astype(jnp.float32)
    query_wide = query_heads.astype(jnp.float32)
    log_keep = jax.nn.log_sigmoid(forget_gate)
    cum_ahead = jnp.cumsum(log_keep[0], axis=-1)
    cum_behind = lax.cumsum(log_keep[1], axis=1, reverse=True)
    ahead = summarize(keys_scaled, values_wide, input_gate[0], cum_ahead, cum_ahead[:, -1])
    behind = summarize(keys_scaled, values_wide, input_gate[1], cum_behind, cum_behind[:, 0])
    ahead_state = entering(ahead, "sp", 1)
    behind_state = entering(behind, "sp", -1)
    scores = jnp.einsum(
        "thd,shd->hts", query_heads, keys_heads, preferred_element_type=jnp.float32
    ) * QK_DIM ** (-0.5)
    lower = jnp.tril(jnp.ones((length, length), dtype=bool))
    both = 0.0
    for way, cum, mask, state in (
        (0, cum_ahead, lower, ahead_state),
        (1, cum_behind, lower.T, behind_state),
    ):
        exponent, block_top = own_block(input_gate[way], cum, mask)
        both = both + read_out(query_wide, scores, value_heads, exponent, block_top, cum, state)
    scaled = both * lax.rsqrt(jnp.mean(both * both, axis=-1, keepdims=True) + epsilon)
    scaled = scaled * head_gain.reshape(heads_here, V_DIM)[:, None, :]
    side_by_side = jnp.transpose(scaled, (1, 0, 2)).reshape(length, heads_here * V_DIM)
    return (side_by_side * jax.nn.sigmoid(out_gate.astype(jnp.float32))).astype(jnp.bfloat16)


def smear(upper, before, after, taps):
    length = upper.shape[1]
    padded = jnp.concatenate([before, upper, after], axis=1)
    total = padded[:, 0:length] * taps[0]
    for offset in range(1, CONV):
        total = total + padded[:, offset : offset + length] * taps[offset]
    return total


def local(
    residual,
    query,
    keys,
    values,
    out_gate,
    input_gate,
    forget_gate,
    head_gain,
    w_out,
    norm_gain,
    w_up_gate,
    w_up_value,
    conv_gate,
    conv_value,
    w_down,
):
    tp, mine = lax.axis_size("tp"), lax.axis_index("tp")
    grp, group = lax.axis_size("grp"), lax.axis_index("grp")
    rows, width = residual.shape
    length = query.shape[0]
    units = w_up_gate.shape[1] // grp

    def unit_share(x, dim):
        return lax.dynamic_slice_in_dim(x, group * units, units, axis=dim)

    gate_whole = lax.all_gather(unit_share(w_up_gate, 1), "sp", axis=0, tiled=True)
    value_whole = lax.all_gather(unit_share(w_up_value, 1), "sp", axis=0, tiled=True)
    down_whole = lax.all_gather(unit_share(w_down, 0), "sp", axis=1, tiled=True)

    w_far = swap(w_out, "tp", 2)
    w_near = swap(w_out, "tp", 1)
    w_pieces = [w_out, w_near, w_far, swap(w_far, "tp", 1)]

    gated = heads_part(query, keys, values, out_gate, input_gate, forget_gate, head_gain)
    blocks = gated.reshape(tp, rows, gated.shape[1])
    projected = jnp.dot(pick(blocks, mine, 0), w_pieces[0], preferred_element_type=jnp.float32)
    for distance in range(1, tp):
        piece = swap(pick(blocks, mine ^ distance, 0), "tp", distance)
        projected = projected + jnp.dot(
            piece, w_pieces[distance], preferred_element_type=jnp.float32
        )
    stream = (residual.astype(jnp.float32) + projected).astype(jnp.bfloat16)
    stream_wide = stream.astype(jnp.float32)
    normed = stream_wide * lax.rsqrt(
        jnp.mean(stream_wide * stream_wide, axis=-1, keepdims=True) + epsilon
    )
    normed = (normed * norm_gain).astype(jnp.bfloat16)

    near, far = mine % 2, mine // 2
    pair = jnp.stack([normed, swap(normed, "grp", 1)], axis=0)
    quad = in_order(pair, swap(pair, "tp", 2), far, 1)
    whole = in_order(quad, swap(quad, "tp", 1), near, 2)
    whole = whole.reshape(grp * length, width)

    def share_up(weight):
        upper = jnp.dot(whole, weight, preferred_element_type=jnp.float32).astype(jnp.bfloat16)
        return upper.reshape(grp, length, units)

    smeared, edges = [], []
    uppers = [share_up(gate_whole), share_up(value_whole)]
    for upper in uppers:
        edges.append((upper[:, -1:], upper[:, :1]))
    last = jnp.concatenate([e[0] for e in edges], axis=-1)
    initial = jnp.concatenate([e[1] for e in edges], axis=-1)
    before = shifted(last, "sp", 1)
    after = shifted(initial, "sp", -1)
    for place, (upper, taps) in enumerate(zip(uppers, (conv_gate, conv_value))):
        cut = slice(place * units, (place + 1) * units)
        smeared.append(smear(upper, before[..., cut], after[..., cut], unit_share(taps, 1)))
    hidden = (jax.nn.silu(smeared[0]) * smeared[1]).astype(jnp.bfloat16)

    hidden = hidden.reshape(grp, tp // 2, 2, rows, units)

    def down(part):
        flat = part.reshape(-1, units)
        terms = jnp.dot(flat, down_whole, preferred_element_type=jnp.float32)
        return terms.reshape(part.shape[:-1] + (width,))

    sent = down(pick(hidden, 1 - near, 2)).astype(jnp.bfloat16)
    got = swap(sent, "tp", 1)
    total = down(pick(hidden, near, 2)) + got.astype(jnp.float32)
    got = swap(pick(total, 1 - far, 1).astype(jnp.bfloat16), "tp", 2)
    total = pick(total, far, 1) + got.astype(jnp.float32)
    got = swap(total[1].astype(jnp.bfloat16), "grp", 1)
    returned = total[0] + got.astype(jnp.float32)
    return (stream_wide + returned).astype(jnp.bfloat16)


def solution(mesh):
    placed = (
        P(("grp", "sp", "tp"), None),
        P(("grp", "sp"), "tp"),
        P(("grp", "sp"), "tp"),
        P(("grp", "sp"), "tp"),
        P(("grp", "sp"), "tp"),
        P(None, "tp", ("grp", "sp")),
        P(None, "tp", ("grp", "sp")),
        P("tp"),
        P("tp", None),
        P(),
        P("sp", "tp"),
        P("sp", "tp"),
        P(None, "tp"),
        P(None, "tp"),
        P("tp", "sp"),
    )
    return jax.shard_map(
        local, mesh=mesh, in_specs=placed, out_specs=P(("grp", "sp", "tp"), None), check_vma=False
    )
```

```python
import jax
import jax.numpy as jnp
from jax import lax
from jax.sharding import PartitionSpec as P

QK_DIM = 128
V_DIM = 256
CONV = 3


epsilon = 1e-06
floor_log = -1e30
highest = lax.Precision.HIGHEST


def swap(x, axis, distance):
    size = lax.axis_size(axis)
    return lax.ppermute(x, axis, [(i, i ^ distance) for i in range(size)])


def shifted(x, axis, distance):
    size = lax.axis_size(axis)
    pairs = [(i, i + distance) for i in range(size) if 0 <= i + distance < size]
    return lax.ppermute(x, axis, pairs)


def pick(x, index, dim):
    return lax.dynamic_index_in_dim(x, index, axis=dim, keepdims=False)


def in_order(mine, other, bit, dim):
    first = jnp.where(bit == 0, mine, other)
    second = jnp.where(bit == 0, other, mine)
    return jnp.stack([first, second], axis=dim)


def combine(early, later):
    early_total, early_memory, early_normalizer, early_top = early
    later_total, later_memory, later_normalizer, later_top = later
    carried = early_top + later_total
    joint_top = jnp.maximum(carried, later_top)
    early_scale = jnp.exp(carried - joint_top)
    later_scale = jnp.exp(later_top - joint_top)
    memory = early_scale[:, None, None] * early_memory + later_scale[:, None, None] * later_memory
    normalizer = early_scale[:, None] * early_normalizer + later_scale[:, None] * later_normalizer
    return (early_total + later_total, memory, normalizer, joint_top)


def pack(state):
    total, memory, normalizer, top = state
    heads, _, width = memory.shape
    row = jnp.pad(normalizer, ((0, 0), (0, width - normalizer.shape[1])))
    scalars = jnp.pad(jnp.stack([total, top], axis=1), ((0, 0), (0, width - 2)))
    extra = jnp.stack([row, scalars], axis=1)
    return jnp.concatenate([memory, jnp.pad(extra, ((0, 0), (0, 6), (0, 0)))], axis=1)


def unpack(packed, present):
    memory = packed[:, :QK_DIM]
    normalizer = packed[:, QK_DIM, :QK_DIM]
    total = packed[:, QK_DIM + 1, 0]
    top = jnp.where(present, packed[:, QK_DIM + 1, 1], floor_log)
    return (total, memory, normalizer, top)


def entering(state, axis, sign):
    size, mine = lax.axis_size(axis), lax.axis_index(axis)
    place = mine if sign > 0 else size - 1 - mine
    window, result, step = state, None, 1
    while step < size:
        got = unpack(shifted(pack(window), axis, sign * step), place >= step)
        result = got if result is None else combine(got, result)
        step *= 2
        if step < size:
            window = combine(got, window)
    return result


def summarize(keys_scaled, values_wide, in_gate, log_cum, totals):
    growth = totals[:, None] - log_cum + in_gate
    largest = jnp.max(growth, axis=-1)
    weighting = jnp.exp(growth - largest[:, None])
    weighted = keys_scaled * jnp.transpose(weighting)[:, :, None]
    memory = jnp.einsum("shd,she->hde", weighted, values_wide, precision=highest)
    return (totals, memory, jnp.sum(weighted, axis=0), largest)


def own_block(in_gate, log_cum, mask):
    exponent = jnp.where(
        mask[None], log_cum[:, :, None] - log_cum[:, None, :] + in_gate[:, None, :], -jnp.inf
    )
    return exponent, jnp.max(exponent, axis=-1)


def read_out(query_wide, scores, value_heads, exponent, block_top, log_cum, state):
    memory, normalizer, top_in = (state[1], state[2], state[3])
    before = log_cum + top_in[:, None]
    running = jnp.maximum(before, block_top)
    carry_scale = jnp.exp(before - running)
    weights = jnp.exp(exponent - running[:, :, None]) * scores
    numerator = carry_scale[:, :, None] * jnp.einsum(
        "thd,hde->hte", query_wide, memory, precision=highest
    )
    numerator = numerator + jnp.einsum(
        "hts,she->hte",
        weights.astype(jnp.bfloat16),
        value_heads,
        preferred_element_type=jnp.float32,
    )
    denominator = carry_scale * jnp.einsum(
        "thd,hd->ht", query_wide, normalizer, precision=highest
    ) + jnp.sum(weights, axis=-1)
    return numerator / jnp.maximum(jnp.abs(denominator), jnp.exp(-running))[:, :, None]


def heads_part(query, keys, values, out_gate, input_gate, forget_gate, head_gain):
    length = query.shape[0]
    heads_here = input_gate.shape[1]
    query_heads = query.reshape(length, heads_here, QK_DIM)
    keys_heads = keys.reshape(length, heads_here, QK_DIM)
    value_heads = values.reshape(length, heads_here, V_DIM)
    keys_scaled = keys_heads.astype(jnp.float32) * QK_DIM ** (-0.5)
    values_wide = value_heads.astype(jnp.float32)
    query_wide = query_heads.astype(jnp.float32)
    log_keep = jax.nn.log_sigmoid(forget_gate)
    cum_ahead = jnp.cumsum(log_keep[0], axis=-1)
    cum_behind = lax.cumsum(log_keep[1], axis=1, reverse=True)
    ahead = summarize(keys_scaled, values_wide, input_gate[0], cum_ahead, cum_ahead[:, -1])
    behind = summarize(keys_scaled, values_wide, input_gate[1], cum_behind, cum_behind[:, 0])
    ahead_state = entering(ahead, "sp", 1)
    behind_state = entering(behind, "sp", -1)
    scores = jnp.einsum(
        "thd,shd->hts", query_heads, keys_heads, preferred_element_type=jnp.float32
    ) * QK_DIM ** (-0.5)
    lower = jnp.tril(jnp.ones((length, length), dtype=bool))
    both = 0.0
    for way, cum, mask, state in (
        (0, cum_ahead, lower, ahead_state),
        (1, cum_behind, lower.T, behind_state),
    ):
        exponent, block_top = own_block(input_gate[way], cum, mask)
        both = both + read_out(query_wide, scores, value_heads, exponent, block_top, cum, state)
    scaled = both * lax.rsqrt(jnp.mean(both * both, axis=-1, keepdims=True) + epsilon)
    scaled = scaled * head_gain.reshape(heads_here, V_DIM)[:, None, :]
    side_by_side = jnp.transpose(scaled, (1, 0, 2)).reshape(length, heads_here * V_DIM)
    return (side_by_side * jax.nn.sigmoid(out_gate.astype(jnp.float32))).astype(jnp.bfloat16)


def smear(upper, before, after, taps):
    length = upper.shape[1]
    padded = jnp.concatenate([before, upper, after], axis=1)
    total = padded[:, 0:length] * taps[0]
    for offset in range(1, CONV):
        total = total + padded[:, offset : offset + length] * taps[offset]
    return total


def local(
    residual,
    query,
    keys,
    values,
    out_gate,
    input_gate,
    forget_gate,
    head_gain,
    w_out,
    norm_gain,
    w_up_gate,
    w_up_value,
    conv_gate,
    conv_value,
    w_down,
):
    tp, mine = lax.axis_size("tp"), lax.axis_index("tp")
    grp, group = lax.axis_size("grp"), lax.axis_index("grp")
    rows, width = residual.shape
    length = query.shape[0]
    units = w_up_gate.shape[1] // grp

    def unit_share(x, dim):
        return lax.dynamic_slice_in_dim(x, group * units, units, axis=dim)

    up_share = jnp.concatenate([unit_share(w_up_gate, 1), unit_share(w_up_value, 1)], axis=1)
    up_whole = lax.all_gather(up_share, "sp", axis=0, tiled=True)
    down_whole = lax.all_gather(unit_share(w_down, 0), "sp", axis=1, tiled=True)

    w_far = swap(w_out, "tp", 2)
    w_near = swap(w_out, "tp", 1)
    w_pieces = [w_out, w_near, w_far, swap(w_far, "tp", 1)]

    gated = heads_part(query, keys, values, out_gate, input_gate, forget_gate, head_gain)
    blocks = gated.reshape(tp, rows, gated.shape[1])
    projected = jnp.dot(pick(blocks, mine, 0), w_pieces[0], preferred_element_type=jnp.float32)
    for distance in range(1, tp):
        piece = swap(pick(blocks, mine ^ distance, 0), "tp", distance)
        projected = projected + jnp.dot(
            piece, w_pieces[distance], preferred_element_type=jnp.float32
        )
    stream = (residual.astype(jnp.float32) + projected).astype(jnp.bfloat16)
    stream_wide = stream.astype(jnp.float32)
    normed = stream_wide * lax.rsqrt(
        jnp.mean(stream_wide * stream_wide, axis=-1, keepdims=True) + epsilon
    )
    normed = (normed * norm_gain).astype(jnp.bfloat16)

    near, far = mine % 2, mine // 2
    pair = jnp.stack([normed, swap(normed, "grp", 1)], axis=0)
    quad = in_order(pair, swap(pair, "tp", 2), far, 1)
    whole = in_order(quad, swap(quad, "tp", 1), near, 2)
    whole = whole.reshape(grp * length, width)

    upper = jnp.dot(whole, up_whole, preferred_element_type=jnp.float32).astype(jnp.bfloat16)
    upper = upper.reshape(grp, length, 2 * units)
    taps = jnp.concatenate([unit_share(conv_gate, 1), unit_share(conv_value, 1)], axis=1)
    before = shifted(upper[:, -1:], "sp", 1)
    after = shifted(upper[:, :1], "sp", -1)
    smeared = smear(upper, before, after, taps)
    hidden = (jax.nn.silu(smeared[..., :units]) * smeared[..., units:]).astype(jnp.bfloat16)

    hidden = hidden.reshape(grp, tp // 2, 2, rows, units)
    hidden_sent = pick(hidden, 1 - near, 2).reshape(-1, units)
    hidden_kept = pick(hidden, near, 2).reshape(-1, units)
    halves = (down_whole[:, : width // 2], down_whole[:, width // 2 :])

    def down(part, weight):
        terms = jnp.dot(part, weight, preferred_element_type=jnp.float32)
        return terms.reshape(grp, tp // 2, rows, width // 2)

    def over_far(total, dim):
        got = swap(pick(total, 1 - far, dim).astype(jnp.bfloat16), "tp", 2)
        return pick(total, far, dim) + got.astype(jnp.float32)

    def over_group(total):
        got = swap(total[1].astype(jnp.bfloat16), "grp", 1)
        return total[0] + got.astype(jnp.float32)

    gots = [swap(down(hidden_sent, half).astype(jnp.bfloat16), "tp", 1) for half in halves]
    totals = [
        down(hidden_kept, half) + got.astype(jnp.float32) for half, got in zip(halves, gots)
    ]
    first = over_group(over_far(totals[0], 1))
    second = over_far(over_group(totals[1]), 0)
    returned = jnp.concatenate([first, second], axis=1)
    return (stream_wide + returned).astype(jnp.bfloat16)


def solution(mesh):
    placed = (
        P(("grp", "sp", "tp"), None),
        P(("grp", "sp"), "tp"),
        P(("grp", "sp"), "tp"),
        P(("grp", "sp"), "tp"),
        P(("grp", "sp"), "tp"),
        P(None, "tp", ("grp", "sp")),
        P(None, "tp", ("grp", "sp")),
        P("tp"),
        P("tp", None),
        P(),
        P("sp", "tp"),
        P("sp", "tp"),
        P(None, "tp"),
        P(None, "tp"),
        P("tp", "sp"),
    )
    return jax.shard_map(
        local, mesh=mesh, in_specs=placed, out_specs=P(("grp", "sp", "tp"), None), check_vma=False
    )
```

```python
import jax
import jax.numpy as jnp
from jax import lax
from jax.sharding import PartitionSpec as P

QK_DIM = 128
V_DIM = 256
CONV = 3


epsilon = 1e-06
floor_log = -1e30
highest = lax.Precision.HIGHEST


def swap(x, axis, distance):
    size = lax.axis_size(axis)
    return lax.ppermute(x, axis, [(i, i ^ distance) for i in range(size)])


def shifted(x, axis, distance):
    size = lax.axis_size(axis)
    pairs = [(i, i + distance) for i in range(size) if 0 <= i + distance < size]
    return lax.ppermute(x, axis, pairs)


def pick(x, index, dim):
    return lax.dynamic_index_in_dim(x, index, axis=dim, keepdims=False)


def in_order(mine, other, bit, dim):
    first = jnp.where(bit == 0, mine, other)
    second = jnp.where(bit == 0, other, mine)
    return jnp.stack([first, second], axis=dim)


def combine(early, later):
    early_total, early_memory, early_normalizer, early_top = early
    later_total, later_memory, later_normalizer, later_top = later
    carried = early_top + later_total
    joint_top = jnp.maximum(carried, later_top)
    early_scale = jnp.exp(carried - joint_top)
    later_scale = jnp.exp(later_top - joint_top)
    memory = early_scale[:, None, None] * early_memory + later_scale[:, None, None] * later_memory
    normalizer = early_scale[:, None] * early_normalizer + later_scale[:, None] * later_normalizer
    return (early_total + later_total, memory, normalizer, joint_top)


def pack(state):
    total, memory, normalizer, top = state
    heads, _, width = memory.shape
    row = jnp.pad(normalizer, ((0, 0), (0, width - normalizer.shape[1])))
    scalars = jnp.pad(jnp.stack([total, top], axis=1), ((0, 0), (0, width - 2)))
    extra = jnp.stack([row, scalars], axis=1)
    return jnp.concatenate([memory, jnp.pad(extra, ((0, 0), (0, 6), (0, 0)))], axis=1)


def unpack(packed, present):
    memory = packed[:, :QK_DIM]
    normalizer = packed[:, QK_DIM, :QK_DIM]
    total = packed[:, QK_DIM + 1, 0]
    top = jnp.where(present, packed[:, QK_DIM + 1, 1], floor_log)
    return (total, memory, normalizer, top)


def entering(state, axis, sign):
    size, mine = lax.axis_size(axis), lax.axis_index(axis)
    place = mine if sign > 0 else size - 1 - mine
    window, result, step = state, None, 1
    while step < size:
        got = unpack(shifted(pack(window), axis, sign * step), place >= step)
        result = got if result is None else combine(got, result)
        step *= 2
        if step < size:
            window = combine(got, window)
    return result


def summarize(keys_scaled, values_wide, in_gate, log_cum, totals):
    growth = totals[:, None] - log_cum + in_gate
    largest = jnp.max(growth, axis=-1)
    weighting = jnp.exp(growth - largest[:, None])
    weighted = keys_scaled * jnp.transpose(weighting)[:, :, None]
    memory = jnp.einsum("shd,she->hde", weighted, values_wide, precision=highest)
    return (totals, memory, jnp.sum(weighted, axis=0), largest)


def own_block(in_gate, log_cum, mask):
    exponent = jnp.where(
        mask[None], log_cum[:, :, None] - log_cum[:, None, :] + in_gate[:, None, :], -jnp.inf
    )
    return exponent, jnp.max(exponent, axis=-1)


def read_out(query_wide, scores, value_heads, exponent, block_top, log_cum, state):
    memory, normalizer, top_in = (state[1], state[2], state[3])
    before = log_cum + top_in[:, None]
    running = jnp.maximum(before, block_top)
    carry_scale = jnp.exp(before - running)
    weights = jnp.exp(exponent - running[:, :, None]) * scores
    numerator = carry_scale[:, :, None] * jnp.einsum(
        "thd,hde->hte", query_wide, memory, precision=highest
    )
    numerator = numerator + jnp.einsum(
        "hts,she->hte",
        weights.astype(jnp.bfloat16),
        value_heads,
        preferred_element_type=jnp.float32,
    )
    denominator = carry_scale * jnp.einsum(
        "thd,hd->ht", query_wide, normalizer, precision=highest
    ) + jnp.sum(weights, axis=-1)
    return numerator / jnp.maximum(jnp.abs(denominator), jnp.exp(-running))[:, :, None]


def heads_part(query, keys, values, out_gate, input_gate, forget_gate, head_gain):
    length = query.shape[0]
    heads_here = input_gate.shape[1]
    query_heads = query.reshape(length, heads_here, QK_DIM)
    keys_heads = keys.reshape(length, heads_here, QK_DIM)
    value_heads = values.reshape(length, heads_here, V_DIM)
    keys_scaled = keys_heads.astype(jnp.float32) * QK_DIM ** (-0.5)
    values_wide = value_heads.astype(jnp.float32)
    query_wide = query_heads.astype(jnp.float32)
    log_keep = jax.nn.log_sigmoid(forget_gate)
    cum_ahead = jnp.cumsum(log_keep[0], axis=-1)
    cum_behind = lax.cumsum(log_keep[1], axis=1, reverse=True)
    ahead = summarize(keys_scaled, values_wide, input_gate[0], cum_ahead, cum_ahead[:, -1])
    behind = summarize(keys_scaled, values_wide, input_gate[1], cum_behind, cum_behind[:, 0])
    ahead_state = entering(ahead, "sp", 1)
    behind_state = entering(behind, "sp", -1)
    scores = jnp.einsum(
        "thd,shd->hts", query_heads, keys_heads, preferred_element_type=jnp.float32
    ) * QK_DIM ** (-0.5)
    lower = jnp.tril(jnp.ones((length, length), dtype=bool))
    both = 0.0
    for way, cum, mask, state in (
        (0, cum_ahead, lower, ahead_state),
        (1, cum_behind, lower.T, behind_state),
    ):
        exponent, block_top = own_block(input_gate[way], cum, mask)
        both = both + read_out(query_wide, scores, value_heads, exponent, block_top, cum, state)
    scaled = both * lax.rsqrt(jnp.mean(both * both, axis=-1, keepdims=True) + epsilon)
    scaled = scaled * head_gain.reshape(heads_here, V_DIM)[:, None, :]
    side_by_side = jnp.transpose(scaled, (1, 0, 2)).reshape(length, heads_here * V_DIM)
    return (side_by_side * jax.nn.sigmoid(out_gate.astype(jnp.float32))).astype(jnp.bfloat16)


def smear(upper, before, after, taps):
    length = upper.shape[1]
    padded = jnp.concatenate([before, upper, after], axis=1)
    total = padded[:, 0:length] * taps[0]
    for offset in range(1, CONV):
        total = total + padded[:, offset : offset + length] * taps[offset]
    return total


def local(
    residual,
    query,
    keys,
    values,
    out_gate,
    input_gate,
    forget_gate,
    head_gain,
    w_out,
    norm_gain,
    w_up_gate,
    w_up_value,
    conv_gate,
    conv_value,
    w_down,
):
    tp, mine = lax.axis_size("tp"), lax.axis_index("tp")
    grp, group = lax.axis_size("grp"), lax.axis_index("grp")
    rows, width = residual.shape
    length = query.shape[0]
    units = w_up_gate.shape[1] // grp

    def unit_share(x, dim):
        return lax.dynamic_slice_in_dim(x, group * units, units, axis=dim)

    up_share = jnp.concatenate([unit_share(w_up_gate, 1), unit_share(w_up_value, 1)], axis=1)
    up_share, w_out, query, keys, values, input_gate, forget_gate = lax.optimization_barrier(
        (up_share, w_out, query, keys, values, input_gate, forget_gate)
    )
    up_whole = lax.all_gather(up_share, "sp", axis=0, tiled=True)
    down_whole = lax.all_gather(unit_share(w_down, 0), "sp", axis=1, tiled=True)

    w_far = swap(w_out, "tp", 2)
    w_near = swap(w_out, "tp", 1)
    w_pieces = [w_out, w_near, w_far, swap(w_far, "tp", 1)]

    gated = heads_part(query, keys, values, out_gate, input_gate, forget_gate, head_gain)
    blocks = gated.reshape(tp, rows, gated.shape[1])
    projected = jnp.dot(pick(blocks, mine, 0), w_pieces[0], preferred_element_type=jnp.float32)
    for distance in range(1, tp):
        piece = swap(pick(blocks, mine ^ distance, 0), "tp", distance)
        projected = projected + jnp.dot(
            piece, w_pieces[distance], preferred_element_type=jnp.float32
        )
    stream = (residual.astype(jnp.float32) + projected).astype(jnp.bfloat16)
    stream_wide = stream.astype(jnp.float32)
    normed = stream_wide * lax.rsqrt(
        jnp.mean(stream_wide * stream_wide, axis=-1, keepdims=True) + epsilon
    )
    normed = (normed * norm_gain).astype(jnp.bfloat16)

    near, far = mine % 2, mine // 2
    pair = jnp.stack([normed, swap(normed, "grp", 1)], axis=0)
    quad = in_order(pair, swap(pair, "tp", 2), far, 1)
    whole = in_order(quad, swap(quad, "tp", 1), near, 2)
    whole = whole.reshape(grp * length, width)

    upper = jnp.dot(whole, up_whole, preferred_element_type=jnp.float32).astype(jnp.bfloat16)
    upper = upper.reshape(grp, length, 2 * units)
    taps = jnp.concatenate([unit_share(conv_gate, 1), unit_share(conv_value, 1)], axis=1)
    before = shifted(upper[:, -1:], "sp", 1)
    after = shifted(upper[:, :1], "sp", -1)
    smeared = smear(upper, before, after, taps)
    hidden = (jax.nn.silu(smeared[..., :units]) * smeared[..., units:]).astype(jnp.bfloat16)

    hidden = hidden.reshape(grp, tp // 2, 2, rows, units)
    hidden_sent = pick(hidden, 1 - near, 2).reshape(-1, units)
    hidden_kept = pick(hidden, near, 2).reshape(-1, units)
    halves = (down_whole[:, : width // 2], down_whole[:, width // 2 :])

    def down(part, weight):
        terms = jnp.dot(part, weight, preferred_element_type=jnp.float32)
        return terms.reshape(grp, tp // 2, rows, width // 2)

    def over_far(total, dim):
        got = swap(pick(total, 1 - far, dim).astype(jnp.bfloat16), "tp", 2)
        return pick(total, far, dim) + got.astype(jnp.float32)

    def over_group(total):
        got = swap(total[1].astype(jnp.bfloat16), "grp", 1)
        return total[0] + got.astype(jnp.float32)

    gots = [swap(down(hidden_sent, half).astype(jnp.bfloat16), "tp", 1) for half in halves]
    totals = [
        down(hidden_kept, half) + got.astype(jnp.float32) for half, got in zip(halves, gots)
    ]
    first = over_group(over_far(totals[0], 1))
    second = over_far(over_group(totals[1]), 0)
    returned = jnp.concatenate([first, second], axis=1)
    return (stream_wide + returned).astype(jnp.bfloat16)


def solution(mesh):
    placed = (
        P(("grp", "sp", "tp"), None),
        P(("grp", "sp"), "tp"),
        P(("grp", "sp"), "tp"),
        P(("grp", "sp"), "tp"),
        P(("grp", "sp"), "tp"),
        P(None, "tp", ("grp", "sp")),
        P(None, "tp", ("grp", "sp")),
        P("tp"),
        P("tp", None),
        P(),
        P("sp", "tp"),
        P("sp", "tp"),
        P(None, "tp"),
        P(None, "tp"),
        P("tp", "sp"),
    )
    return jax.shard_map(
        local, mesh=mesh, in_specs=placed, out_specs=P(("grp", "sp", "tp"), None), check_vma=False
    )
```
